32 devices in a mesh: sp: 8 (over z, core), tp: 4 (over y, x).
Axes of the slice: x: 2, y: 2, z: 4, core: 2. Of those that a mesh axis runs over, the one named last changes fastest.
Arguments:
- stream: bfloat16 [3072, 2048], P('sp', 'tp'), may hold values from -6 to 6
- doc_ids: int32 [3072], P('sp'), may hold values from 0 to 1, never falling along the last dimension, each value on 1 to 2304 neighbouring positions
- w_value: bfloat16 [3, 2048, 2048], P(None, None, 'tp'), may hold values from -0.125 to 0.125
- w_gate: bfloat16 [3, 2048, 2048], P(None, None, 'tp'), may hold values from -0.125 to 0.125
- conv_kernel: bfloat16 [3, 31, 2048], P(None, None, 'tp'), may hold values from -4 to 4
- conv_gain: float32 [3, 2048], replicated, may hold values from 0.1 to 1.9
- conv_shift: float32 [3, 2048], replicated, may hold values from -3 to 3
- w_proj: bfloat16 [3, 2048, 2048], P(None, None, 'tp'), may hold values from -0.125 to 0.125
- out_gain: float32 [3, 2048], replicated, may hold values from 0.1 to 1.9
- out_shift: float32 [3, 2048], replicated, may hold values from -3 to 3
Outputs:
- result: bfloat16 [3072, 2048], P('sp', 'tp')
The draws below stay inside these ranges and needn't reach their ends.
All inputs are finite; a program needn't handle non-finite values.
Results may differ from the reference program's by a relative error of at most 0.013.
Values may be sent and summed in bfloat16 or wider, within the bound.
No kernel may reach another device: no remote copies, remote signals or barrier semaphores. Data moves between devices by JAX's collectives and lax.ppermute only.
A program may use at most 64 MiB of HBM per device.

```python
import math
import jax
import jax.numpy as jnp
import numpy as np
from jax import lax

D = 2048
DC = 2048
KERNEL = 31
LAYERS = 3
TOK_DEV = 384
HALF = 15
TOKENS = 3072


def draw_conv_kernel(key, part):
    first = jax.random.fold_in(key, 11)
    second = jax.random.fold_in(key, 12)
    rough = jax.random.uniform(second, (DC,), jnp.float32, 0.5, 1.5)
    base = jnp.clip(jax.random.normal(first, (LAYERS, KERNEL, DC), jnp.float32), -4.0, 4.0)
    ramp = jnp.exp(jnp.linspace(math.log(0.4), math.log(2.0), DC))
    return (base * (ramp * rough)[None, None, :] * KERNEL ** (-0.5)).astype(jnp.bfloat16)


def steps_of(rng, shape, pieces, smallest, largest):
    def one(axis_at, shards_of):
        steps = jax.random.uniform(jax.random.fold_in(jax.random.fold_in(rng, 6), axis_at), (shards_of,), jnp.float32, smallest / len(pieces), largest / len(pieces))
        return jnp.repeat(jnp.exp(steps), shape[axis_at] // shards_of).reshape((-1,) + (1,) * (len(shape) - axis_at - 1))

    level = one(*pieces[0])
    for cut in pieces[1:]:
        level = level * one(*cut)
    return level


def split_up(count, total, reach, slope):
    loads = [(1 << 20) // math.isqrt(grade ** slope) + 1 for grade in range(2, count + 1)]
    surplus, counts = total - reach - (count - 1), [1] * (count - 1)
    while surplus > 0:
        free = [i for i in range(count - 1) if counts[i] < reach]
        pool, left = sum([loads[i] for i in free]), surplus
        for i in free:
            more = min(reach - counts[i], max(1, left * loads[i] // pool), surplus)
            counts[i] = counts[i] + more
            surplus = surplus - more
    return np.array([reach] + counts)


def ragged(key, amount, total, limit, lean):
    if amount == 2:
        one = jax.random.randint(key, (), max(1, total - limit), min(limit, total - 1) + 1)
        return jnp.stack([one, total - one])
    lengths = jnp.asarray(split_up(amount, total, limit, lean), jnp.int32)
    twos = (amount - 1) // 2
    donor, sink = lengths[1:1 + 2 * twos:2], lengths[2:2 + 2 * twos:2]
    slack = jnp.minimum(donor - 1, limit - sink)
    passed = jax.random.randint(jax.random.fold_in(key, 1), (twos,), 0, 1 << 20) % (slack + 1)
    lengths = lengths.at[1:1 + 2 * twos:2].set(donor - passed).at[2:2 + 2 * twos:2].set(sink + passed)
    return lengths[jax.random.permutation(jax.random.fold_in(key, 2), amount)]


def bell_draw(own_key, extent, scale, limit, shards=(), held_as=jnp.bfloat16):
    level = steps_of(own_key, extent, shards, -0.22, 0.18) if shards else 1.0
    drawn = jax.random.normal(own_key, extent, jnp.float32) * scale * level
    return jnp.minimum(jnp.maximum(drawn, -limit), limit).astype(held_as)


def setup_inputs(seed: int = 0) -> dict:
    arg_keys = jax.random.split(jax.random.key(seed), 11)
    stream = bell_draw(arg_keys[0], (TOKENS, D), 1.0, 6.0, ((0, 8), (1, 4)))
    doc_ids = jnp.searchsorted(jnp.cumsum(ragged(arg_keys[1], TOKENS // (3 * TOK_DEV), TOKENS, 6 * TOK_DEV, 2)), jnp.arange(TOKENS), side="right").astype(jnp.int32)
    w_value = bell_draw(arg_keys[2], (LAYERS, D, DC), D ** -0.5, 0.125, ((2, 4),))
    w_gate = bell_draw(arg_keys[3], (LAYERS, D, DC), D ** -0.5, 0.125, ((2, 4),))
    conv_kernel = draw_conv_kernel(jax.random.fold_in(arg_keys[10], 71), 0)
    conv_gain = jnp.clip(1.0 + 0.18 * jax.random.normal(arg_keys[5], (LAYERS, DC), jnp.float32), 0.1, 1.9)
    conv_shift = bell_draw(arg_keys[6], (LAYERS, DC), 0.5, 3.0, (), jnp.float32)
    w_proj = bell_draw(arg_keys[7], (LAYERS, DC, D), DC ** -0.5, 0.125, ((2, 4),))
    out_gain = jnp.clip(1.0 + 0.18 * jax.random.normal(arg_keys[8], (LAYERS, D), jnp.float32), 0.1, 1.9)
    out_shift = bell_draw(arg_keys[9], (LAYERS, D), 0.5, 3.0, (), jnp.float32)
    return dict(stream=stream, doc_ids=doc_ids, w_value=w_value, w_gate=w_gate, conv_kernel=conv_kernel, conv_gain=conv_gain, conv_shift=conv_shift, w_proj=w_proj, out_gain=out_gain, out_shift=out_shift)


ALPHA = 2.0 ** 0.25
EPS = 1e-05

def reference(stream, doc_ids, w_value, w_gate, conv_kernel, conv_gain, conv_shift, w_proj, out_gain, out_shift):
    hidden = stream
    seg_pad = jnp.pad(doc_ids, (HALF, HALF), constant_values=-1)
    for layer in range(LAYERS):
        lin = jnp.dot(hidden, w_value[layer], preferred_element_type=jnp.float32)
        gat = jnp.dot(hidden, w_gate[layer], preferred_element_type=jnp.float32)
        glu = (lin * jax.nn.sigmoid(gat)).astype(jnp.bfloat16)
        padded = jnp.pad(glu.astype(jnp.float32), ((HALF, HALF), (0, 0)))
        taps = conv_kernel[layer].astype(jnp.float32)
        total = jnp.zeros((TOKENS, DC), jnp.float32)
        for k in range(KERNEL):
            keep = (seg_pad[k:k + TOKENS] == doc_ids).astype(jnp.float32)[:, None]
            total = total + padded[k:k + TOKENS] * keep * taps[k][None, :]
        conv = total.astype(jnp.bfloat16).astype(jnp.float32)
        centre = lax.optimization_barrier(jnp.mean(conv, axis=1, keepdims=True))
        spread = lax.optimization_barrier(jnp.mean(jnp.square(conv - centre), axis=1, keepdims=True))
        normed = (conv - centre) * jax.lax.rsqrt(spread + EPS) * conv_gain[layer] + conv_shift[layer]
        act = jax.nn.silu(normed).astype(jnp.bfloat16)
        mixed = ALPHA * hidden.astype(jnp.float32) + jnp.dot(act, w_proj[layer], preferred_element_type=jnp.float32)
        mean_z = lax.optimization_barrier(jnp.mean(mixed, axis=1, keepdims=True))
        var_z = lax.optimization_barrier(jnp.mean(jnp.square(mixed - mean_z), axis=1, keepdims=True))
        hidden = ((mixed - mean_z) * jax.lax.rsqrt(var_z + EPS) * out_gain[layer] + out_shift[layer]).astype(jnp.bfloat16)
    return hidden
```

```python
import functools

import jax
import jax.numpy as jnp
from jax import lax
from jax.experimental import pallas as pl
from jax.experimental.pallas import tpu as pltpu
from jax.sharding import PartitionSpec as P

KERNEL = 31
LAYERS = 3
HALF = 15
EDGE = 16
BLOCK = 16

ALPHA = 2.0**0.25
EPS = 1e-05
F32 = jnp.float32
BF16 = jnp.bfloat16


VMEM = pl.BlockSpec(memory_space=pltpu.VMEM)
SMEM = pl.BlockSpec(memory_space=pltpu.SMEM)
HBM = pl.BlockSpec(memory_space=pltpu.HBM)
PARAMS = pltpu.CompilerParams(vmem_limit_bytes=50 * 1024 * 1024)


def shape(dims, dtype):
    return jax.ShapeDtypeStruct(dims, dtype)


def spread_to_group(piece):
    count = lax.axis_size("tp")
    if count != 4:
        return "all", (lax.all_gather(piece, "tp", axis=0),)
    places = [(sp, tp) for sp in range(lax.axis_size("sp")) for tp in range(count)]
    early = [(sp * count + tp, sp * count + (tp ^ (1 + sp % 2))) for sp, tp in places]
    late = [(sp * count + tp, sp * count + (tp ^ (2 - sp % 2))) for sp, tp in places]
    one = lax.ppermute(piece, ("sp", "tp"), early)
    two = lax.ppermute(jnp.stack([piece, one]), ("sp", "tp"), late)
    return "pairs", (piece, one, two)


def piece_readers(mode, refs, group):
    if mode == "all":
        (whole,) = refs
        return [(j, (lambda lo, n, j=j: whole[j, lo : lo + n, :])) for j in range(group)]
    own, one, two = refs
    me = lax.axis_index("tp")
    early = 1 + lax.axis_index("sp") % 2
    return [
        (me, lambda lo, n: own[lo : lo + n, :]),
        (me ^ early, lambda lo, n: one[lo : lo + n, :]),
        (me ^ (3 - early), lambda lo, n: two[0, lo : lo + n, :]),
        (me ^ 3, lambda lo, n: two[1, lo : lo + n, :]),
    ]


def fetch(source, layer, target, sems, at):
    half = target.shape[0] // 2
    copies = []
    for i in range(2):
        rows = pl.ds(i * half, half)
        copies.append(
            pltpu.make_async_copy(source.at[layer, rows, :], target.at[rows, :], sems.at[at + i])
        )
    return copies


def row_norm(readers, lo, n, width):
    total = None
    for _, read in readers:
        part = jnp.sum(read(lo, n).astype(F32), axis=1, keepdims=True)
        total = part if total is None else total + part
    mean = total * (1.0 / width)
    total = None
    for _, read in readers:
        part = jnp.sum(jnp.square(read(lo, n).astype(F32) - mean), axis=1, keepdims=True)
        total = part if total is None else total + part
    return mean, lax.rsqrt(total * (1.0 / width) + EPS)


def sigmoid(v):
    return 0.5 * jnp.tanh(0.5 * v) + 0.5


def glu_body(*refs, mode, pieces, group, layer, rows, norm):
    refs = list(refs)
    piece_refs = [refs.pop(0) for _ in range(pieces)]
    value_hbm, gate_hbm = refs.pop(0), refs.pop(0)
    if norm:
        gain, shift = refs.pop(0), refs.pop(0)
    glu_out = refs.pop(0)
    hidden_out = refs.pop(0) if norm else None
    wide, value_w, gate_w, sems = refs
    local = wide.shape[1] // group
    width = wide.shape[1]
    value_copies = fetch(value_hbm, layer, value_w, sems, 0)
    gate_copies = fetch(gate_hbm, layer, gate_w, sems, 2)
    for copy in (value_copies[0], gate_copies[0], value_copies[1], gate_copies[1]):
        copy.start()
    readers = piece_readers(mode, piece_refs, group)
    for lo in range(0, rows, BLOCK):
        if norm:
            mean, scale = row_norm(readers, lo, BLOCK, width)
        for index, read in readers:
            value = read(lo, BLOCK)
            if norm:
                value = (value.astype(F32) - mean) * scale * gain[index] + shift[index]
                value = value.astype(BF16)
            start = index * local
            if not isinstance(start, int):
                start = pl.multiple_of(start, 128)
            wide[lo : lo + BLOCK, pl.ds(start, local)] = value
    if norm:
        mine = pl.multiple_of(lax.axis_index("tp") * local, 128)
        hidden_out[...] = wide[:, pl.ds(mine, local)]
    lin, gat = None, None
    half = width // 2
    for i in range(2):
        cols = slice(i * half, (i + 1) * half)
        value_copies[i].wait()
        gate_copies[i].wait()
        part = jnp.dot(wide[:, cols], value_w[cols, :], preferred_element_type=F32)
        lin = part if lin is None else lin + part
        part = jnp.dot(wide[:, cols], gate_w[cols, :], preferred_element_type=F32)
        gat = part if gat is None else gat + part
    glu_out[...] = (lin * sigmoid(gat)).astype(BF16)


def glu_call(mode, arrays, value_all, gate_all, gain, shift, layer):
    group = lax.axis_size("tp")
    rows, local = arrays[0].shape[-2:]
    norm = gain is not None
    width = value_all.shape[1]
    operands = [*arrays, value_all, gate_all] + ([gain, shift] if norm else [])
    specs = [VMEM] * len(arrays) + [HBM, HBM] + ([VMEM, VMEM] if norm else [])
    outs = [shape((rows, local), BF16)] * (2 if norm else 1)
    body = functools.partial(
        glu_body, mode=mode, pieces=len(arrays), group=group, layer=layer, rows=rows, norm=norm
    )
    res = pl.pallas_call(
        body,
        out_shape=outs,
        in_specs=specs,
        out_specs=[VMEM] * len(outs),
        scratch_shapes=[
            pltpu.VMEM((rows, width), BF16),
            pltpu.VMEM((width, local), BF16),
            pltpu.VMEM((width, local), BF16),
            pltpu.SemaphoreType.DMA((4,)),
        ],
        compiler_params=PARAMS,
        cost_estimate=pl.CostEstimate(
            flops=4 * rows * width * local, bytes_accessed=4 * width * local, transcendentals=0
        ),
        name="glu",
    )(*operands)
    return (res[0], res[1]) if norm else (res[0], None)


def conv_window(window, taps, out, out_at, rows, flags, codes, row_at):
    local = out.shape[1]
    lanes = min(128, local)
    for c in range(0, local, lanes):
        total = None
        for s in range(8):
            n = rows + (8 if s else 0)
            acc = None
            for j in range(4):
                m = 8 * j + s
                if not 1 <= m <= KERNEL:
                    continue
                term = window[8 * j : 8 * j + n, c : c + lanes] * taps[m - 1 : m, c : c + lanes]
                acc = term if acc is None else acc + term
            acc = acc[s : s + rows]
            total = acc if total is None else total + acc
        out[out_at : out_at + rows, c : c + lanes] = total.astype(BF16)

    def fix(b, carry):
        @pl.when(flags[row_at // BLOCK + b] != 0)
        def _():
            at = pl.multiple_of(b * BLOCK, BLOCK)
            code = codes[pl.ds(pl.multiple_of(row_at + b * BLOCK, BLOCK), BLOCK), :]
            first = code & 255
            last = (KERNEL - 1) - (code >> 8)
            for c in range(0, local, lanes):
                span = window[pl.ds(at, BLOCK + 2 * EDGE), c : c + lanes]
                total = jnp.zeros((BLOCK, lanes), F32)
                for k in range(KERNEL):
                    keep = (first <= k) & (last >= k)
                    term = span[k + 1 : k + 1 + BLOCK] * taps[k : k + 1, c : c + lanes]
                    total = total + jnp.where(keep[:, :lanes], term, 0.0)
                out[pl.ds(pl.multiple_of(out_at + b * BLOCK, BLOCK), BLOCK), c : c + lanes] = (
                    total.astype(BF16)
                )

        return carry

    lax.fori_loop(0, rows // BLOCK, fix, 0)


def outer_conv_body(flags, codes, taps_ref, low, glu, high, out, win, taps, *, total_rows):
    half = glu.shape[0] // 2
    rows = half - EDGE
    taps[...] = taps_ref[...].astype(F32)
    win[0:EDGE, :] = low[...].astype(F32)
    win[EDGE : EDGE + half, :] = glu[0:half, :].astype(F32)
    conv_window(win.at[0 : half + EDGE], taps, out, 0, rows, flags, codes, 0)
    base = half + EDGE
    win[base : base + half, :] = glu[half:, :].astype(F32)
    win[base + half : base + half + EDGE, :] = high[...].astype(F32)
    conv_window(
        win.at[base : base + half + EDGE], taps, out, rows, rows, flags, codes, total_rows - rows
    )


def inner_conv_body(flags, codes, taps_ref, outer, glu, out, win, taps, *, total_rows):
    half = outer.shape[0] // 2
    inner = glu.shape[0]
    rows = inner + 2 * EDGE
    taps[...] = taps_ref[...].astype(F32)
    win[0 : 2 * EDGE, :] = outer[half - 2 * EDGE : half, :].astype(F32)
    win[2 * EDGE : 2 * EDGE + inner, :] = glu[...].astype(F32)
    win[2 * EDGE + inner :, :] = outer[half : half + 2 * EDGE, :].astype(F32)
    conv_window(win, taps, out, 0, rows, flags, codes, half - EDGE)


def conv_call(body, flags, codes, taps, blocks, rows, window, total_rows):
    local = taps.shape[1]
    return pl.pallas_call(
        functools.partial(body, total_rows=total_rows),
        out_shape=shape((rows, local), BF16),
        in_specs=[SMEM, VMEM, VMEM] + [VMEM] * len(blocks),
        out_specs=VMEM,
        scratch_shapes=[pltpu.VMEM((window, local), F32), pltpu.VMEM(taps.shape, F32)],
        compiler_params=PARAMS,
        cost_estimate=pl.CostEstimate(
            flops=512 * rows * local * KERNEL, bytes_accessed=4 * rows * local, transcendentals=0
        ),
        name="conv",
    )(flags, codes, taps, *blocks)


def proj_body(*refs, mode, pieces, group, layer, rows, residual, last):
    refs = list(refs)
    piece_refs = [refs.pop(0) for _ in range(pieces)]
    hidden = [refs.pop(0) for _ in residual]
    proj_hbm, gain, shift = refs.pop(0), refs.pop(0), refs.pop(0)
    z_out = refs.pop(0)
    stat_out = refs.pop(0) if last else None
    wide, proj_w, sems = refs
    local = wide.shape[1] // group
    width = wide.shape[1]
    copies = fetch(proj_hbm, layer, proj_w, sems, 0)
    for copy in copies:
        copy.start()
    readers = piece_readers(mode, piece_refs, group)
    for lo in range(0, rows, BLOCK):
        mean, scale = row_norm(readers, lo, BLOCK, width)
        for index, read in readers:
            value = (read(lo, BLOCK).astype(F32) - mean) * scale * gain[index] + shift[index]
            start = index * local
            if not isinstance(start, int):
                start = pl.multiple_of(start, 128)
            wide[lo : lo + BLOCK, pl.ds(start, local)] = (value * sigmoid(value)).astype(BF16)
    for copy in copies:
        copy.wait()
    branch = jnp.dot(wide[...], proj_w[...], preferred_element_type=F32)
    at = 0
    for ref, spans in zip(hidden, residual):
        for src, dst, n in spans:
            z = ALPHA * ref[src : src + n, :].astype(F32) + branch[dst : dst + n]
            if not last:
                z_out[dst : dst + n, :] = z.astype(BF16)
                continue
            z_out[dst : dst + n, :] = z
            mean = jnp.sum(z, axis=1, keepdims=True) * (1.0 / local)
            spread = jnp.sum(jnp.square(z - mean), axis=1, keepdims=True)
            lane = lax.broadcasted_iota(jnp.int32, (n, 128), 1)
            stat_out[dst : dst + n, :] = jnp.where(lane == 0, mean, jnp.where(lane == 1, spread, 0.0))


def proj_call(mode, arrays, hidden, residual, proj_all, gain, shift, layer, last):
    group = lax.axis_size("tp")
    rows, local = arrays[0].shape[-2:]
    width = proj_all.shape[1]
    outs = [shape((rows, local), F32 if last else BF16)]
    if last:
        outs.append(shape((rows, 128), F32))
    body = functools.partial(
        proj_body,
        mode=mode,
        pieces=len(arrays),
        group=group,
        layer=layer,
        rows=rows,
        residual=residual,
        last=last,
    )
    res = pl.pallas_call(
        body,
        out_shape=outs,
        in_specs=[VMEM] * (len(arrays) + len(hidden)) + [HBM, VMEM, VMEM],
        out_specs=[VMEM] * len(outs),
        scratch_shapes=[
            pltpu.VMEM((rows, width), BF16),
            pltpu.VMEM((width, local), BF16),
            pltpu.SemaphoreType.DMA((2,)),
        ],
        compiler_params=PARAMS,
        cost_estimate=pl.CostEstimate(
            flops=4 * rows * width * local, bytes_accessed=4 * width * local, transcendentals=0
        ),
        name="proj",
    )(*arrays, *hidden, proj_all, gain, shift)
    return res


def group_stats(stat):
    count = lax.axis_size("tp")
    mine = stat[:, :2].T
    if count == 4:
        one = lax.ppermute(mine, "tp", [(i, i ^ 1) for i in range(count)])
        both = jnp.stack([mine, one])
        two = lax.ppermute(both, "tp", [(i, i ^ 2) for i in range(count)])
        return jnp.concatenate([both, two])
    return lax.all_gather(mine, "tp", axis=0)


def finish(z, stat, gain, shift, local, width):
    every = group_stats(stat)
    means, spreads = every[:, 0], every[:, 1]
    mean = jnp.mean(means, axis=0)
    spread = jnp.sum(spreads, axis=0) + local * jnp.sum(jnp.square(means - mean), axis=0)
    scale = lax.rsqrt(spread / width + EPS)
    return ((z - mean[:, None]) * scale[:, None] * gain + shift).astype(BF16)


def on_device(
    stream,
    doc_ids,
    w_value,
    w_gate,
    conv_kernel,
    conv_gain,
    conv_shift,
    w_proj,
    out_gain,
    out_shift,
):
    rows, local = stream.shape
    width = w_value.shape[1]
    group = lax.axis_size("tp")
    sp_count = lax.axis_size("sp")
    sp = lax.axis_index("sp")
    tp = lax.axis_index("tp")
    forward = [(i, i + 1) for i in range(sp_count - 1)]
    backward = [(i + 1, i) for i in range(sp_count - 1)]

    half = rows // 4 + EDGE * (LAYERS - 1)
    state = (jnp.concatenate([stream[:half], stream[rows - half :]]), stream[half : rows - half])
    gathered = [spread_to_group(part) for part in state]
    hidden = state

    low_ids = lax.ppermute(doc_ids[rows - EDGE :], "sp", forward)
    high_ids = lax.ppermute(doc_ids[:EDGE], "sp", backward)
    low_ids = jnp.where(sp == 0, doc_ids[0], low_ids)
    high_ids = jnp.where(sp == sp_count - 1, doc_ids[rows - 1], high_ids)
    ids = jnp.concatenate([low_ids, doc_ids, high_ids])
    before = sum((ids[EDGE - d : EDGE - d + rows] != doc_ids) for d in range(1, HALF + 1))
    after = sum((ids[EDGE + d : EDGE + d + rows] != doc_ids) for d in range(1, HALF + 1))
    code = (before + 256 * after).astype(jnp.int32)
    flags = jnp.max(code.reshape(rows // BLOCK, BLOCK), axis=1)
    codes = jnp.broadcast_to(code[:, None], (rows, 128))

    def by_piece(table):
        return table.reshape(LAYERS, group, 1, local)

    conv_gain, conv_shift = by_piece(conv_gain), by_piece(conv_shift)
    out_gain, out_shift = by_piece(out_gain), by_piece(out_shift)

    for layer in range(LAYERS):
        gain = out_gain[layer - 1] if layer else None
        shift = out_shift[layer - 1] if layer else None
        glu_a, hid_a = glu_call(*gathered[0], w_value, w_gate, gain, shift, layer)
        low = lax.ppermute(glu_a[2 * half - EDGE :], "sp", forward)
        high = lax.ppermute(glu_a[:EDGE], "sp", backward)
        conv_a = conv_call(
            outer_conv_body,
            flags,
            codes,
            conv_kernel[layer],
            (low, glu_a, high),
            2 * (half - EDGE),
            2 * (half + EDGE),
            rows,
        )
        over_a = spread_to_group(conv_a)
        inner = rows - 2 * half
        glu_b, hid_b = glu_call(*gathered[1], w_value, w_gate, gain, shift, layer)
        conv_b = conv_call(
            inner_conv_body,
            flags,
            codes,
            conv_kernel[layer],
            (glu_a, glu_b),
            inner + 2 * EDGE,
            inner + 4 * EDGE,
            rows,
        )
        over_b = spread_to_group(conv_b)
        if layer:
            hidden = (hid_a, hid_b)
        keep = half - EDGE
        last = layer == LAYERS - 1
        out_a = proj_call(
            *over_a,
            (hidden[0],),
            (((0, 0, keep), (half + EDGE, keep, keep)),),
            w_proj,
            conv_gain[layer],
            conv_shift[layer],
            layer,
            last,
        )
        out_b = proj_call(
            *over_b,
            hidden,
            (((keep, 0, EDGE), (half, EDGE + inner, EDGE)), ((0, EDGE, inner),)),
            w_proj,
            conv_gain[layer],
            conv_shift[layer],
            layer,
            last,
        )
        half = keep
        if not last:
            state = (out_a[0], out_b[0])
            gathered = [spread_to_group(part) for part in state]

    gain = lax.dynamic_index_in_dim(out_gain[LAYERS - 1], tp, 0, keepdims=False)
    shift = lax.dynamic_index_in_dim(out_shift[LAYERS - 1], tp, 0, keepdims=False)
    done_a = finish(*out_a, gain, shift, local, width)
    done_b = finish(*out_b, gain, shift, local, width)
    return jnp.concatenate([done_a[:half], done_b, done_a[half:]])


def solution(mesh):
    in_specs = (
        P("sp", "tp"),
        P("sp"),
        P(None, None, "tp"),
        P(None, None, "tp"),
        P(None, None, "tp"),
        P(),
        P(),
        P(None, None, "tp"),
        P(),
        P(),
    )
    out_specs = P("sp", "tp")
    return jax.shard_map(
        on_device, mesh=mesh, in_specs=in_specs, out_specs=out_specs, check_vma=False
    )
```
